128 devices in a mesh: sp: 16 (over z, x), dp: 8 (over y, core).
Axes of the slice: x: 4, y: 4, z: 4, core: 2. Of those that a mesh axis runs over, the one named last changes fastest.
Arguments:
- query_input: bfloat16 [8, 8192, 2048], P('dp', 'sp'), may hold values from -6 to 6
- forget_gate_input: bfloat16 [8, 8192, 2048], P('dp', 'sp'), may hold values from -6.5 to 6.5
- value_input: bfloat16 [8, 8192, 2048], P('dp', 'sp'), may hold values from -6 to 6
- gate_input: bfloat16 [8, 8192, 2048], P('dp', 'sp'), may hold values from -6 to 6
- extra_decay: bfloat16 [8, 8192, 2048], P('dp', 'sp'), may hold values from -0.7 to 0
- floor_gap: float32 [2048], replicated, may hold values from 0 to 0.06
- norm_gain: float32 [2048], replicated, may hold values from 0.1 to 1.9
- out_weight: bfloat16 [2048, 4096], P(None, 'dp'), may hold values from -0.125 to 0.125
Outputs:
- mixed_out: bfloat16 [8, 8192, 4096], P('dp', 'sp')
The draws below stay inside these ranges and needn't reach their ends.
All inputs are finite; a program needn't handle non-finite values.
Results may differ from the reference program's by a relative error of at most 0.0049.
Values may be sent and summed in bfloat16 or wider, within the bound.
No kernel may reach another device: no remote copies, remote signals or barrier semaphores. Data moves between devices by JAX's collectives and lax.ppermute only.
A program may use at most 192 MiB of HBM per device.

```python
import jax
import jax.numpy as jnp
from jax import lax

D = 4096
HW = 2048
HEAD_DIM = 128
BLOCK = 128
TOK_DEV = 512
HEADS = 16
SEQUENCE_LENGTH = 8192
SEQS = 8


def draw_forget_gate_input(key, part):
    key_noise = jax.random.fold_in(key, 101)
    key_shift = jax.random.fold_in(key, 102)
    noise_field = jax.random.truncated_normal(key_noise, -5.0, 5.0, (SEQS, SEQUENCE_LENGTH, HW), jnp.float32)
    block_shift = jax.random.uniform(key_shift, (SEQS, SEQUENCE_LENGTH // TOK_DEV, 1, HEADS, 1), jnp.float32, -1.5, 1.5)
    block_shift = jnp.broadcast_to(block_shift, (SEQS, SEQUENCE_LENGTH // TOK_DEV, TOK_DEV, HEADS, HEAD_DIM))
    return (noise_field + block_shift.reshape(SEQS, SEQUENCE_LENGTH, HW)).astype(jnp.bfloat16)


def draw_extra_decay(key, part):
    key_stable_draw = jax.random.fold_in(key, 201)
    key_spots = jax.random.fold_in(key, 202)
    key_loss = jax.random.fold_in(key, 203)
    stable_portion = -jax.random.uniform(key_stable_draw, (SEQS, SEQUENCE_LENGTH, HW), jnp.float32) / SEQUENCE_LENGTH
    sample_places = jax.random.randint(key_spots, (SEQS, 3), 0, SEQUENCE_LENGTH)
    surge_mask = jnp.any(jnp.arange(SEQUENCE_LENGTH)[None, :, None] == sample_places[:, None, :], axis=-1)
    loss_fraction = jax.random.uniform(key_loss, (SEQS, SEQUENCE_LENGTH, HW), jnp.float32, 0.2, 0.5)
    return jnp.where(surge_mask[:, :, None], jnp.log1p(-loss_fraction), stable_portion).astype(jnp.bfloat16)


def draw_floor_gap(key, part):
    key_fast = jax.random.fold_in(key, 301)
    key_quick = jax.random.fold_in(key, 302)
    key_slow = jax.random.fold_in(key, 303)
    fast_share = 0.5
    fast_heads = jax.random.uniform(key_fast, (HEADS, 1), jnp.float32) < fast_share
    quick_gap = jnp.exp(jax.random.uniform(key_quick, (HEADS, HEAD_DIM), jnp.float32, jnp.log(0.02), jnp.log(0.06)))
    slow_gap = jnp.exp(jax.random.uniform(key_slow, (HEADS, HEAD_DIM), jnp.float32, jnp.log(0.1), 0.0)) / SEQUENCE_LENGTH
    return jnp.where(fast_heads, quick_gap, slow_gap).reshape(HW).astype(jnp.float32)


def level_of(own_key, extent, pieces, smallest, high):
    gain, own = 1.0, jax.random.fold_in(own_key, 6)
    for dim, shards_of in pieces:
        heights = jnp.exp(jax.random.uniform(jax.random.fold_in(own, dim), (shards_of,), jnp.float32, smallest / len(pieces), high / len(pieces)))
        gain = gain * jnp.repeat(heights, extent[dim] // shards_of).reshape([-1 if axis == dim else 1 for axis in range(len(extent))])
    return gain


def centred(key, dims, spread, most, shards=(), kind=jnp.bfloat16):
    values = spread * jax.random.normal(key, dims, jnp.float32)
    if shards:
        values = values * level_of(key, dims, shards, -0.22, 0.18)
    return jnp.clip(values, -most, most).astype(kind)


def setup_inputs(seed: int = 0) -> dict:
    key_of = jax.random.split(jax.random.key(seed), 9)
    query_input = centred(key_of[0], (SEQS, SEQUENCE_LENGTH, HW), 1.0, 6.0, ((0, 8), (1, 16)))
    forget_gate_input = draw_forget_gate_input(jax.random.fold_in(key_of[8], 71), 0)
    value_input = centred(key_of[2], (SEQS, SEQUENCE_LENGTH, HW), 1.0, 6.0, ((0, 8), (1, 16)))
    gate_input = centred(key_of[3], (SEQS, SEQUENCE_LENGTH, HW), 1.0, 6.0, ((0, 8), (1, 16)))
    extra_decay = draw_extra_decay(jax.random.fold_in(key_of[8], 71), 0)
    floor_gap = draw_floor_gap(jax.random.fold_in(key_of[8], 71), 0)
    norm_gain = jnp.clip(1.0 + 0.18 * jax.random.normal(key_of[6], (HW,), jnp.float32), 0.1, 1.9)
    out_weight = centred(key_of[7], (HW, D), HW ** -0.5, 0.125, ((1, 8),))
    return dict(query_input=query_input, forget_gate_input=forget_gate_input, value_input=value_input, gate_input=gate_input, extra_decay=extra_decay, floor_gap=floor_gap, norm_gain=norm_gain, out_weight=out_weight)


norm_eps = 1e-06
pairs_per_step = 16
highest = lax.Precision.HIGHEST

def prepare(query_input, forget_gate_input, value_input, extra_decay, floor_gap):
    positions, channels = query_input.shape
    head_shape = (positions, channels // HEAD_DIM, HEAD_DIM)
    queries = jax.nn.silu(query_input.astype(jnp.float32))
    inflow = floor_gap * jax.nn.sigmoid(-forget_gate_input.astype(jnp.float32))
    log_keep = jnp.log1p(-inflow) + extra_decay.astype(jnp.float32)
    value_rows = value_input.astype(jnp.float32)
    return (queries.reshape(head_shape), inflow.reshape(head_shape), log_keep.reshape(head_shape), value_rows.reshape(head_shape))

def block_parts(queries, inflow, log_keep, value_rows):
    positions, head_count, head_width = queries.shape
    block_count = positions // BLOCK
    pair_count = block_count * head_count
    causal = jnp.tril(jnp.ones((BLOCK, BLOCK), dtype=bool))

    def to_pairs(tensor):
        paired = tensor.reshape(block_count, BLOCK, head_count, head_width).transpose(0, 2, 1, 3)
        return paired.reshape(pair_count // pairs_per_step, pairs_per_step, BLOCK, head_width)

    def group_terms(operands):
        query_grp, inflow_grp, keep_grp, value_grp = operands
        running = jnp.cumsum(keep_grp, axis=1)
        decayed = query_grp * jnp.exp(running)
        boosted = inflow_grp * jnp.exp(-running)
        scores = jnp.einsum('gtk,gsk->gts', decayed, boosted, precision=highest)
        scores = jnp.where(causal[None], scores, 0.0)
        inner = jnp.einsum('gts,gsv->gtv', scores, value_grp, precision=highest)
        latest = running[:, -1, :]
        weighted = inflow_grp * jnp.exp(latest[:, None, :] - running)
        block_state = jnp.einsum('gsk,gsv->gkv', weighted, value_grp, precision=highest)
        return (inner, decayed, block_state, jnp.exp(latest))
    inner, decayed, block_state, block_fade = lax.map(group_terms, (to_pairs(queries), to_pairs(inflow), to_pairs(log_keep), to_pairs(value_rows)))
    return (inner.reshape(block_count, head_count, BLOCK, head_width), decayed.reshape(block_count, head_count, BLOCK, head_width), block_state.reshape(block_count, head_count, head_width, head_width), block_fade.reshape(block_count, head_count, head_width))

def finish(inner, decayed, prior_states, gate_input, norm_gain):
    block_count, head_count, block_len, head_width = inner.shape
    result = inner + jnp.einsum('nhtk,nhkv->nhtv', decayed, prior_states, precision=highest)
    result = result.transpose(0, 2, 1, 3).reshape(block_count * block_len, head_count, head_width)
    scaled = result * lax.rsqrt(lax.optimization_barrier(jnp.mean(result * result, axis=-1, keepdims=True)) + norm_eps)
    scaled = scaled.reshape(block_count * block_len, head_count * head_width)
    scaled = scaled * norm_gain * jax.nn.silu(gate_input.astype(jnp.float32))
    return scaled.astype(jnp.bfloat16)

def reference(query_input, forget_gate_input, value_input, gate_input, extra_decay, floor_gap, norm_gain, out_weight):

    def one_sequence(member):
        query_one, forget_one, value_one, gate_one, extra_one = member
        queries, inflow, log_keep, value_rows = prepare(query_one, forget_one, value_one, extra_one, floor_gap)
        inner, decayed, block_state, block_fade = block_parts(queries, inflow, log_keep, value_rows)

        def carry_step(state, operands):
            fresh, fading = operands
            return (fading[..., None] * state + fresh, state)
        _, prior_states = lax.scan(carry_step, jnp.zeros(block_state.shape[1:], jnp.float32), (block_state, block_fade))
        hidden = finish(inner, decayed, prior_states, gate_one, norm_gain)
        return jnp.dot(hidden, out_weight, preferred_element_type=jnp.float32).astype(jnp.bfloat16)
    return lax.map(one_sequence, (query_input, forget_gate_input, value_input, gate_input, extra_decay))
```

```python
import jax
import jax.numpy as jnp
from jax import lax
from jax.experimental import pallas as pl
from jax.experimental.pallas import tpu as pltpu
from jax.sharding import Mesh
from jax.sharding import PartitionSpec as P

HD = 128
BLOCK = 128
AXES = ("z", "x", "y", "c")

norm_eps = 1e-06
LOG2E = 1.4426950408889634
F32 = jnp.float32
BF16 = jnp.bfloat16
TROWS = HD + 16
ORDER = (2, 1, 3, 0)


def dot_tt(a, b):
    return lax.dot_general(a, b, (((0,), (0,)), ((), ())), preferred_element_type=F32)


def dot_nt(a, b):
    return lax.dot_general(a, b, (((1,), (1,)), ((), ())), preferred_element_type=F32)


def dot_nn(a, b):
    return lax.dot_general(a, b, (((1,), (0,)), ((), ())), preferred_element_type=F32)


def params(limit=None):
    return pltpu.CompilerParams(vmem_limit_bytes=limit)


def state_body(pos, f_ref, e_ref, v_ref, gap_ref, r_ref, b_ref, *outs):
    tokens, width = f_ref.shape
    step = pl.program_id(0)
    blocks = tokens // BLOCK
    row = lax.broadcasted_iota(jnp.int32, (BLOCK, 2 * BLOCK), 0)
    col = lax.broadcasted_iota(jnp.int32, (BLOCK, 2 * BLOCK), 1) % BLOCK
    tri = jnp.where(col <= row, 1.0, 0.0).astype(BF16)
    gap = gap_ref[...]
    later = jnp.zeros((1, width), F32)
    scaled = [None] * blocks
    for b in reversed(range(blocks)):
        rows = pl.ds(b * BLOCK, BLOCK)
        f = f_ref[rows, :].astype(F32)
        inflow = gap / (1.0 + jnp.exp2(f * LOG2E))
        keep = jnp.log2(1.0 - inflow) + e_ref[rows, :].astype(F32) * LOG2E
        hi = keep.astype(BF16)
        lo = (keep - hi.astype(F32)).astype(BF16)
        run = dot_nn(tri, jnp.concatenate([hi, lo], axis=0))
        r_ref[rows, :] = run
        mid = run[BLOCK // 2 - 1 : BLOCK // 2, :]
        last = run[BLOCK - 1 : BLOCK, :]
        boosted = inflow * jnp.exp2(mid - run)
        b_ref[rows, :] = boosted.astype(BF16)
        scaled[b] = (boosted * jnp.exp2(last - mid + later)).astype(BF16)
        later = later + last
    weights = jnp.concatenate(scaled, axis=0)
    fade = jnp.exp2(later)
    fade_hi = fade.astype(BF16)
    fade_lo = (fade - fade_hi.astype(F32)).astype(BF16)
    per = width // HD
    steps = pl.num_programs(0) // 4
    for h in range(per):
        lanes = slice(h * HD, (h + 1) * HD)
        st = dot_tt(v_ref[:, lanes], weights[:, lanes]).astype(BF16)
        tail = jnp.concatenate(
            [
                jnp.broadcast_to(fade_hi[:, lanes], (8, HD)),
                jnp.broadcast_to(fade_lo[:, lanes], (8, HD)),
            ],
            axis=0,
        )
        for j, s in enumerate(ORDER):

            @pl.when(step // steps == j)
            def _():
                slot = (step % steps) * per + h
                outs[s][slot, :HD, :] = st
                outs[s][slot, HD:, :] = tail


def state_stage(pos, f, e, v, gap):
    tokens, channels = f.shape
    width = 256
    grid = channels // width
    steps = grid // 4
    heads_group = channels // HD // 4

    def place(i, pos):
        j = i // steps
        shift = jnp.where(j == 0, ORDER[0], jnp.where(j == 1, ORDER[1], jnp.where(j == 2, ORDER[2], ORDER[3])))
        return ((pos[1] + shift) % 4) * steps + i % steps

    wide = pl.BlockSpec((tokens, width), lambda i, pos: (0, place(i, pos)))
    flat = pl.BlockSpec((1, width), lambda i, pos: (0, place(i, pos)))
    out = pl.BlockSpec((heads_group, TROWS, HD), lambda i, pos: (0, 0, 0))
    piece = jax.ShapeDtypeStruct((heads_group, TROWS, HD), BF16)
    return pl.pallas_call(
        state_body,
        grid_spec=pltpu.PrefetchScalarGridSpec(
            num_scalar_prefetch=1,
            grid=(grid,),
            in_specs=[wide, wide, wide, flat],
            out_specs=[wide, wide] + [out] * 4,
        ),
        out_shape=[
            jax.ShapeDtypeStruct((tokens, channels), F32),
            jax.ShapeDtypeStruct((tokens, channels), BF16),
        ]
        + [piece] * 4,
        compiler_params=params(),
        name="state_stage",
    )(pos, f, e, v, gap)


def inner_body(q_ref, r_ref, b_ref, v_ref, i_ref, d_ref):
    tokens, width = q_ref.shape
    row = lax.broadcasted_iota(jnp.int32, (BLOCK, BLOCK), 0)
    col = lax.broadcasted_iota(jnp.int32, (BLOCK, BLOCK), 1)
    causal = col <= row
    for h in range(width // HD):
        lanes = slice(h * HD, (h + 1) * HD)
        state = None
        before = jnp.zeros((1, HD), F32)
        for b in range(tokens // BLOCK):
            rows = pl.ds(b * BLOCK, BLOCK)
            q = q_ref[rows, lanes].astype(F32)
            q = q / (1.0 + jnp.exp2(q * -LOG2E))
            run = r_ref[rows, lanes]
            mid = run[BLOCK // 2 - 1 : BLOCK // 2, :]
            last = run[BLOCK - 1 : BLOCK, :]
            decayed = q * jnp.exp2(run - mid)
            boosted = b_ref[rows, lanes]
            values = v_ref[rows, lanes]
            scores = dot_nt(decayed.astype(BF16), boosted)
            scores = jnp.where(causal, scores, 0.0).astype(BF16)
            acc = dot_nn(scores, values)
            if b:
                acc = acc + dot_nt((decayed * jnp.exp2(mid)).astype(BF16), state.astype(BF16))
            i_ref[rows, lanes] = acc
            d_ref[rows, lanes] = (decayed * jnp.exp2(mid + before)).astype(BF16)
            before = before + last
            if b + 1 < tokens // BLOCK:
                scaled = (boosted.astype(F32) * jnp.exp2(last - mid)).astype(BF16)
                fresh = dot_tt(values, scaled)
                state = fresh if state is None else state * jnp.exp2(last) + fresh


def inner_stage(q, run, boosted, v):
    tokens, channels = q.shape
    width = 256
    wide = pl.BlockSpec((tokens, width), lambda i: (0, i))
    return pl.pallas_call(
        inner_body,
        grid=(channels // width,),
        in_specs=[wide] * 4,
        out_specs=[wide, wide],
        out_shape=[
            jax.ShapeDtypeStruct((tokens, channels), F32),
            jax.ShapeDtypeStruct((tokens, channels), BF16),
        ],
        compiler_params=params(),
        name="inner_stage",
    )(q, run, boosted, v)


def fade_of(ref, h):
    tail = ref[h, HD:, :].astype(F32)
    return tail[0:1, :] + tail[8:9, :]


def chain(flags, fades):
    total = None
    for flag, fade in zip(flags, fades):
        part = jnp.where(flag, fade, 1.0)
        total = part if total is None else total * part
    return total


def row_body(pos, *refs):
    parts, out = refs[:4], refs[4]
    x = pos[1]
    place = [(x - s) % 4 for s in range(4)]
    for h in range(out.shape[0]):
        fades = [fade_of(p, h) for p in parts]
        total = jnp.zeros((HD, HD), F32)
        for s in range(4):
            after = chain([place[k] > place[s] for k in range(4)], fades)
            total = total + parts[s][h, :HD, :].astype(F32) * after
        out[h, :HD, :] = total.astype(BF16)
        whole = fades[0] * fades[1] * fades[2] * fades[3]
        hi = whole.astype(BF16)
        lo = (whole - hi.astype(F32)).astype(BF16)
        out[h, HD:, :] = jnp.concatenate(
            [jnp.broadcast_to(hi, (8, HD)), jnp.broadcast_to(lo, (8, HD))], axis=0
        )


def small_call(body, pos, args, n_out, shape, name):
    def whole(a):
        return pl.BlockSpec(a.shape, lambda i, pos: (0,) * len(a.shape))

    struct = jax.ShapeDtypeStruct(shape, BF16)
    return pl.pallas_call(
        body,
        grid_spec=pltpu.PrefetchScalarGridSpec(
            num_scalar_prefetch=1,
            grid=(1,),
            in_specs=[whole(a) for a in args],
            out_specs=[whole(struct)] * n_out,
        ),
        out_shape=[struct] * n_out,
        compiler_params=params(),
        name=name,
    )(pos, *args)


def prior_body(pos, *refs):
    parts, rows, outs = refs[:4], refs[4:7], refs[7:]
    z, x = pos[0], pos[1]
    place = [(x - s) % 4 for s in range(4)]
    zplace = [(z - s) % 4 for s in range(1, 4)]
    for h in range(outs[0].shape[0]):
        fades = [fade_of(p, h) for p in parts]
        zfades = [fade_of(p, h) for p in rows]
        enter = jnp.zeros((HD, HD), F32)
        for s in range(3):
            after = chain(
                [(zplace[k] > zplace[s]) & (zplace[k] < z) for k in range(3)], zfades
            )
            after = jnp.where(zplace[s] < z, after, 0.0)
            enter = enter + rows[s][h, :HD, :].astype(F32) * after
        states = [p[h, :HD, :].astype(F32) for p in parts]
        for s in range(4):
            dest = (x + s) % 4
            prior = enter * chain([place[k] < dest for k in range(4)], fades)
            for j in range(4):
                after = chain(
                    [(place[k] > place[j]) & (place[k] < dest) for k in range(4)], fades
                )
                prior = prior + states[j] * jnp.where(place[j] < dest, after, 0.0)
            outs[s][h] = prior.astype(BF16)


N_W = 7


def finish_body(pos, i_ref, d_ref, g_ref, gain_ref, s0, s1, s2, s3, *rest):
    wparts = rest[: 2 * N_W]
    out_ref, hid, wbuf, sems = rest[2 * N_W :]
    step = pl.program_id(0)
    heads = pl.num_programs(0) - 8
    tokens, width = i_ref.shape
    f = pos[4]
    half = hid.shape[1] // 2
    quarter = half // 2

    def spots(side):
        base = 4 * side
        o = side * N_W
        return [
            (o + 0, base + 0, 0, 2 * half),
            (o + 1, base + 1, 0, 2 * half),
            (o + 2, base + 2, 0, half),
            (o + 3, base + 2, half, half),
            (o + 4, base + 3, f * half, half),
            (o + 5, base + 3, (1 - f) * half, quarter),
            (o + 6, base + 3, (1 - f) * half + quarter, quarter),
        ]

    copies = []
    for a, b in zip(spots(0), spots(1)):
        for k, slot, start, size in (a, b):
            copies.append(
                (
                    slot,
                    pltpu.make_async_copy(
                        wparts[k], wbuf.at[slot, pl.ds(start, size), :], sems.at[k]
                    ),
                )
            )

    @pl.when(step == 0)
    def _():
        for _, copy in copies:
            copy.start()

    @pl.when(step < heads)
    def _():
        per = width // HD
        group_steps = heads // 4
        group = step // group_steps
        first = (step % group_steps) * per
        block = ((pos[1] - group) % 4) * group_steps + step % group_steps
        for h in range(per):
            lanes = slice(h * HD, (h + 1) * HD)
            st = jnp.where(
                group == 0,
                s0[first + h],
                jnp.where(group == 1, s1[first + h], jnp.where(group == 2, s2[first + h], s3[first + h])),
            )
            rec = i_ref[:, lanes] + dot_nt(d_ref[:, lanes], st)
            scale = lax.rsqrt(jnp.mean(rec * rec, axis=1, keepdims=True) + norm_eps)
            gate = g_ref[:, lanes].astype(F32)
            gate = gate / (1.0 + jnp.exp2(gate * -LOG2E))
            res = rec * scale * gain_ref[:, lanes] * gate
            hid[:, pl.ds(pl.multiple_of(block * width + h * HD, HD), HD)] = res.astype(BF16)

    for n in range(8):
        slot = (n % 2) * 4 + n // 2

        @pl.when(step == heads + n)
        def _():
            for s, copy in copies:
                if s == slot:
                    copy.wait()
            out_ref[...] = dot_nn(hid[...], wbuf[slot]).astype(BF16)


def finish_stage(pos, inner, decayed, gate, gain, states, wparts, out_cols):
    tokens, channels = inner.shape
    width = 256
    heads = channels // width
    group_steps = heads // 4

    def place(i, pos):
        i = jnp.minimum(i, heads - 1)
        return ((pos[1] - i // group_steps) % 4) * group_steps + i % group_steps

    def column(i, pos):
        n = jnp.maximum(i - heads, 0)
        side = n % 2
        k = n // 2
        y, c, f = pos[2], pos[3], pos[4]
        core = jnp.where(side == 0, c, 1 - c)
        near = jnp.where((core + f) % 2 == 0, 3, 1)
        shift = jnp.where(k == 0, 0, jnp.where(k == 1, near, jnp.where(k == 2, 4 - near, 2)))
        return ((y + shift) % 4) * 2 + core

    wide = pl.BlockSpec((tokens, width), lambda i, pos: (0, place(i, pos)))
    flat = pl.BlockSpec((1, width), lambda i, pos: (0, place(i, pos)))
    st = pl.BlockSpec(states[0].shape, lambda i, pos: (0, 0, 0))
    anyspace = pl.BlockSpec(memory_space=pl.ANY)
    cols = out_cols // 8
    return pl.pallas_call(
        finish_body,
        grid_spec=pltpu.PrefetchScalarGridSpec(
            num_scalar_prefetch=1,
            grid=(heads + 8,),
            in_specs=[wide, wide, wide, flat] + [st] * 4 + [anyspace] * (2 * N_W),
            out_specs=pl.BlockSpec((tokens, cols), lambda i, pos: (0, column(i, pos))),
            scratch_shapes=[
                pltpu.VMEM((tokens, channels), BF16),
                pltpu.VMEM((8, channels, cols), BF16),
                pltpu.SemaphoreType.DMA((2 * N_W,)),
            ],
        ),
        out_shape=jax.ShapeDtypeStruct((tokens, out_cols), BF16),
        compiler_params=params(50 * 2**20),
        name="finish_stage",
    )(pos, inner, decayed, gate, gain, *states, *wparts)


def every():
    for z in range(4):
        for x in range(4):
            for y in range(4):
                for c in range(2):
                    yield z, x, y, c


def flat_id(z, x, y, c):
    return (((z % 4) * 4 + x % 4) * 4 + y % 4) * 2 + c


def along_y():
    pairs = []
    for z, x, y, c in every():
        step = 1 if (c + z + x) % 2 == 0 else -1
        pairs.append((flat_id(z, x, y, c), flat_id(z, x, y + step, c)))
    return pairs


def along_x():
    return [(flat_id(z, x, y, c), flat_id(z, x + 1 - 2 * c, y, c)) for z, x, y, c in every()]


def along_z():
    return [(flat_id(z, x, y, c), flat_id(z + 1 - 2 * c, x, y, c)) for z, x, y, c in every()]


def gather_weight(weight, parity):
    rows = weight.shape[0]
    half, quarter = rows // 2, rows // 4
    near = lax.ppermute(weight, AXES, along_y())
    far = lax.ppermute(lax.dynamic_slice_in_dim(near, parity * half, half, 0), AXES, along_y())
    x1 = lax.ppermute(near[:half], AXES, along_x())
    z1 = lax.ppermute(near[half:], AXES, along_z())
    x2 = lax.ppermute(far[:quarter], AXES, along_x())
    z2 = lax.ppermute(far[quarter:], AXES, along_z())
    mine = [weight, near, x1, z1, far, x2, z2]
    other = [lax.ppermute(piece, "c", [(0, 1), (1, 0)]) for piece in mine]
    return mine + other


def ring(shift):
    return [(i, (i + shift) % 4) for i in range(4)]


def shards(query, forget, value, gate, extra, floor_gap, norm_gain, weight):
    z, x, y, c = (lax.axis_index(a) for a in AXES)
    parity = (z + x) % 2
    index = lax.iota(jnp.int32, 8)
    pos = jnp.zeros(8, jnp.int32)
    for n, v in enumerate((z, x, y, c, parity)):
        pos = jnp.where(index == n, v, pos)
    wparts = gather_weight(weight, parity)
    run, boosted, p0, p1, p2, p3 = state_stage(
        pos, forget[0], extra[0], value[0], floor_gap[None]
    )
    a2 = lax.ppermute(p2, "x", ring(2))
    a1 = lax.ppermute(p1, "x", ring(1))
    a3 = lax.ppermute(p3, "x", ring(3))
    inner, decayed = inner_stage(query[0], run, boosted, value[0])
    parts = (p0, a1, a2, a3)
    (total,) = small_call(row_body, pos, parts, 1, p0.shape, "row_stage")
    rows = [lax.ppermute(total, "z", ring(s)) for s in (1, 2, 3)]
    priors = small_call(
        prior_body, pos, (*parts, *rows), 4, (p0.shape[0], HD, HD), "prior_stage"
    )
    states = [priors[0]] + [lax.ppermute(priors[s], "x", ring(s)) for s in (1, 2, 3)]
    out = finish_stage(
        pos, inner, decayed, gate[0], norm_gain[None], states, wparts, weight.shape[1] * 8
    )
    return out[None]


def solution(mesh):
    split = Mesh(mesh.devices.reshape(4, 4, 4, 2), AXES)
    tokens = P(("y", "c"), ("z", "x"), None)
    placed = (tokens,) * 5 + (P(), P(), P(None, ("y", "c")))
    return jax.shard_map(
        shards, mesh=split, in_specs=placed, out_specs=tokens, check_vma=False
    )
```
